512 devices in a mesh: fs: 16 (over y, x), tp: 32 (over z, core).
Axes of the slice: x: 4, y: 4, z: 16, core: 2. Of those that a mesh axis runs over, the one named last changes fastest.
Arguments:
- normed: bfloat16 [2048, 49152], P('tp', 'fs'), may hold values from -6 to 6
- key_cot: bfloat16 [2048, 49152], P('tp', 'fs'), may hold values from -6 to 6
- first_map: bfloat16 [2048, 49152], P('tp', 'fs'), may hold values from -6 to 6
- second_map: bfloat16 [2048, 49152], P('tp', 'fs'), may hold values from -6 to 6
- lambdas: float32 [8], replicated, may hold values from 0.3 to 0.8
- factor: bfloat16 [2048, 256], replicated, may hold values from -0.125 to 0.125
- key_master: float32 [2048, 2048], P('fs', 'tp'), may hold values from -0.125 to 0.125
- value_master: float32 [2048, 2048], P('fs', 'tp'), may hold values from -0.125 to 0.125
- key_first: float32 [256, 2048], P('fs', 'tp'), may hold values from -6 to 6
- key_second: float32 [256, 2048], P('fs', 'tp'), may hold values from 0.5 to 2
- value_first: float32 [256, 2048], P('fs', 'tp'), may hold values from -6 to 6
- value_second: float32 [256, 2048], P('fs', 'tp'), may hold values from 0.5 to 2
Outputs:
- key_master_new: float32 [2048, 2048], P('fs', 'tp')
- value_master_new: float32 [2048, 2048], P('fs', 'tp')
- key_copy: bfloat16 [2048, 2048], P(None, 'tp')
- value_copy: bfloat16 [2048, 2048], P(None, 'tp')
- key_first_new: float32 [256, 2048], P('fs', 'tp')
- key_second_new: float32 [256, 2048], P('fs', 'tp')
- value_first_new: float32 [256, 2048], P('fs', 'tp')
- value_second_new: float32 [256, 2048], P('fs', 'tp')
The draws below stay inside these ranges and needn't reach their ends.
All inputs are finite; a program needn't handle non-finite values.
Results may differ from the reference program's by a relative error of at most 0.0012.
Values may be sent and summed in bfloat16 or wider, within the bound.
No kernel may reach another device: no remote copies, remote signals or barrier semaphores. Data moves between devices by JAX's collectives and lax.ppermute only.
A program may use at most 64 MiB of HBM per device.

```python
import math
import jax
import jax.numpy as jnp
from jax import lax

D = 2048
HEADS = 8
VALUE_DIM = 256
RANK = 256
TOKENS = 49152
KW = 2048
HV = 2048


def block_levels(rng, extent, cuts, low, high):
    level = 1.0
    for axis_at, shards_of in cuts:
        steps = jax.random.uniform(jax.random.fold_in(jax.random.fold_in(rng, 6), axis_at), (shards_of,), jnp.float32, low / len(cuts), high / len(cuts))
        level = level * jnp.repeat(jnp.exp(steps), extent[axis_at] // shards_of).reshape((-1,) + (1,) * (len(extent) - 1 - axis_at))
    return level


def centred(own_key, shape, width, limit, pieces=(), kind=jnp.bfloat16):
    values = jax.random.normal(own_key, shape, jnp.float32) * width
    if len(pieces) > 0:
        values = block_levels(own_key, shape, pieces, -0.22, 0.18) * values
    return jnp.clip(values, min=-limit, max=limit).astype(kind)


def setup_inputs(seed: int = 0) -> dict:
    splits = jax.random.split(jax.random.key(seed), 13)
    normed = centred(splits[0], (D, TOKENS), 1.0, 6.0, ((0, 32), (1, 16)))
    key_cot = centred(splits[1], (KW, TOKENS), 1.0, 6.0, ((0, 32), (1, 16)))
    first_map = centred(splits[2], (HV, TOKENS), 1.0, 6.0, ((0, 32), (1, 16)))
    second_map = centred(splits[3], (HV, TOKENS), 1.0, 6.0, ((0, 32), (1, 16)))
    lambdas = jnp.clip(jax.random.uniform(splits[4], (HEADS,), jnp.float32, 0.3, 0.8), 0.3, 0.8)
    factor = centred(splits[5], (D, RANK), D ** -0.5, 0.125)
    key_master = centred(splits[6], (D, KW), D ** -0.5, 0.125, ((0, 16), (1, 32)), jnp.float32)
    value_master = centred(splits[7], (D, HV), D ** -0.5, 0.125, ((0, 16), (1, 32)), jnp.float32)
    key_first = centred(splits[8], (RANK, KW), 1.0, 6.0, ((0, 16), (1, 32)), jnp.float32)
    key_second = jnp.clip(jnp.exp(math.log(2.0) - 1.3862944 * jax.random.uniform(splits[9], (RANK, KW), jnp.float32) ** block_levels(splits[9], (RANK, KW), ((0, 16), (1, 32)), -0.2, 0.2)), 0.5, 2.0)
    value_first = centred(splits[10], (RANK, HV), 1.0, 6.0, ((0, 16), (1, 32)), jnp.float32)
    value_second = jnp.clip(jnp.exp(math.log(2.0) - 1.3862944 * jax.random.uniform(splits[11], (RANK, HV), jnp.float32) ** block_levels(splits[11], (RANK, HV), ((0, 16), (1, 32)), -0.2, 0.2)), 0.5, 2.0)
    return dict(normed=normed, key_cot=key_cot, first_map=first_map, second_map=second_map, lambdas=lambdas, factor=factor, key_master=key_master, value_master=value_master, key_first=key_first, key_second=key_second, value_first=value_first, value_second=value_second)


def summed(left, right):
    return lax.dot_general(left, right, (((1,), (1,)), ((), ())), preferred_element_type=jnp.float32)

def advance(gradient, factor32, first, second, master):
    small = lax.dot_general(factor32, gradient, (((0,), (0,)), ((), ())), precision=lax.Precision.HIGHEST)
    first_new = 0.8 * first + 0.2 * small
    second_new = 0.9 * second + 0.1 * small * small
    direction = first_new / (jnp.sqrt(second_new) + 1e-06)
    raw = jnp.dot(factor32, direction, precision=lax.Precision.HIGHEST)
    update = raw / jnp.sqrt(jnp.mean(raw * raw) + 0.01)
    master_new = 0.998 * master - 0.02 * update
    return (master_new, first_new, second_new)

def reference(normed, key_cot, first_map, second_map, lambdas, factor, key_master, value_master, key_first, key_second, value_first, value_second):
    head_lambda = jnp.repeat(lambdas, VALUE_DIM)
    value_cot = (first_map.astype(jnp.float32) - head_lambda[:, None] * second_map.astype(jnp.float32)).astype(jnp.bfloat16)
    norm_scale = 1.0 / jnp.sqrt(jnp.float32(TOKENS))
    key_grad = summed(normed, key_cot) * norm_scale
    value_grad = summed(normed, value_cot) * norm_scale
    factor32 = factor.astype(jnp.float32)
    key_new, key_first_new, key_second_new = advance(key_grad, factor32, key_first, key_second, key_master)
    value_new, value_first_new, value_second_new = advance(value_grad, factor32, value_first, value_second, value_master)
    return (key_new, value_new, key_new.astype(jnp.bfloat16), value_new.astype(jnp.bfloat16), key_first_new, key_second_new, value_first_new, value_second_new)
```

```python
import math

import jax
import jax.numpy as jnp
from jax import lax
from jax.sharding import Mesh
from jax.sharding import PartitionSpec as P

VALUE_DIM = 256
TP = ("tp_0", "tp_1")
FS = ("fs_0", "fs_1")
FS_CORE = ("fs_0", "fs_1", "tp_1")
LINK_SCALE = 32.0


def swap(pieces, axes):
    return lax.all_to_all(pieces, axes, 0, 0, tiled=True)


def to_all(shard, axes):
    size = lax.axis_size(axes)
    return swap(jnp.broadcast_to(shard[None], (size, *shard.shape)), axes)


def in_bf16_parts(values, count):
    parts = []
    for _ in range(count):
        part = lax.reduce_precision(values, 8, 7)
        parts.append(part.astype(jnp.bfloat16))
        values = values - part
    return parts


def local(
    normed,
    key_cot,
    first_map,
    second_map,
    lambdas,
    factor,
    key_master,
    value_master,
    key_first,
    key_second,
    value_first,
    value_second,
):
    width, tokens = normed.shape
    cores = lax.axis_size("tp_1")
    chips = lax.axis_size("tp_0")
    fs_size = lax.axis_size(FS)
    rank = factor.shape[1]
    rows = factor.shape[0]
    heads = lambdas.shape[0]
    fs_rows = key_master.shape[0]
    fs_at = lax.axis_index(FS)
    half = tokens // cores
    share = half // chips

    rows_here = lax.axis_index(TP) * width + lax.iota(jnp.int32, width)
    owners = rows_here // VALUE_DIM
    picked = (owners[:, None] == lax.iota(jnp.int32, heads)[None, :]).astype(jnp.float32)
    row_lambda = jnp.sum(picked * lambdas[None, :], axis=1)
    value_cot = (
        first_map.astype(jnp.float32) - row_lambda[:, None] * second_map.astype(jnp.float32)
    ).astype(jnp.bfloat16)

    stacked = jnp.stack([normed, key_cot, value_cot])
    halves = jnp.stack([stacked[:, :, c * half : (c + 1) * half] for c in range(cores)])
    halves = swap(halves, "tp_1")
    features = halves[:, 0].reshape(cores * width, half)
    cots = halves[:, 1:].reshape(cores * 2 * width, half)

    by_token = features.T.reshape(chips, share, cores * width)
    by_token = swap(by_token, "tp_0")
    product = lax.dot_general(
        by_token.transpose(1, 0, 2).reshape(share, rows),
        factor,
        (((1,), (0,)), ((), ())),
        preferred_element_type=jnp.float32,
    )
    masters_here = jnp.concatenate([key_master.T, value_master.T], axis=0)
    masters, product = lax.optimization_barrier((masters_here, product))
    masters = to_all(masters, FS)
    link = (product * LINK_SCALE).astype(jnp.float16)
    link = lax.all_gather(link, "tp_0", axis=0, tiled=True)

    high, low = in_bf16_parts(link.astype(jnp.float32), 2)
    dims = (((0,), (1,)), ((), ()))
    partial = lax.dot_general(high, cots, dims, preferred_element_type=jnp.float32)
    partial = partial + lax.dot_general(low, cots, dims, preferred_element_type=jnp.float32)
    pieces = partial.reshape(fs_size, rank // fs_size, cores, 2 * width)
    pieces = pieces.transpose(0, 2, 1, 3).reshape(fs_size * cores, rank // fs_size, 2 * width)
    masters, pieces = lax.optimization_barrier((masters, pieces))
    norm_scale = 1.0 / (LINK_SCALE * math.sqrt(tokens * fs_size))
    small = jnp.sum(swap(pieces, FS_CORE), axis=0) * norm_scale

    first = jnp.concatenate([key_first, value_first], axis=1)
    second = jnp.concatenate([key_second, value_second], axis=1)
    first_new = 0.8 * first + 0.2 * small
    second_new = 0.9 * second + 0.1 * small * small
    direction = first_new / (jnp.sqrt(second_new) + 1e-06)
    directions = to_all(direction, FS).reshape(rank, 2 * width)

    raw = sum(
        lax.dot_general(part, factor, (((0,), (1,)), ((), ())), preferred_element_type=jnp.float32)
        for part in in_bf16_parts(directions, 3)
    )
    squares = jnp.stack([jnp.sum(raw[:width] * raw[:width]), jnp.sum(raw[width:] * raw[width:])])
    squares = jnp.sum(to_all(squares.reshape(1, 2), TP), axis=(0, 1))
    cells = rows * width * cores * chips
    scales = 0.02 / jnp.sqrt(squares / cells + 0.01)
    row_scale = jnp.repeat(scales, width)[:, None]
    raw_here = lax.dynamic_slice_in_dim(raw, fs_at * fs_rows, fs_rows, 1)
    new_here = 0.998 * masters_here - row_scale * raw_here
    all_masters = masters.transpose(1, 0, 2).reshape(2 * width, rows)
    copies = (0.998 * all_masters - row_scale * raw).astype(jnp.bfloat16)
    return (
        new_here[:width].T,
        new_here[width:].T,
        copies[:width].T,
        copies[width:].T,
        first_new[:, :width],
        second_new[:, :width],
        first_new[:, width:],
        second_new[:, width:],
    )


def solution(mesh):
    split = Mesh(mesh.devices.reshape(4, 4, 16, 2), ("fs_0", "fs_1", "tp_0", "tp_1"))
    placed = (
        P(TP, FS),
        P(TP, FS),
        P(TP, FS),
        P(TP, FS),
        P(),
        P(),
        P(FS, TP),
        P(FS, TP),
        P(FS, TP),
        P(FS, TP),
        P(FS, TP),
        P(FS, TP),
    )
    return jax.shard_map(
        local,
        mesh=split,
        in_specs=placed,
        out_specs=(
            P(FS, TP),
            P(FS, TP),
            P(None, TP),
            P(None, TP),
            P(FS, TP),
            P(FS, TP),
            P(FS, TP),
            P(FS, TP),
        ),
        check_vma=False,
    )
```

```python
import math

import jax
import jax.numpy as jnp
from jax import lax
from jax.experimental import pallas as pl
from jax.experimental.pallas import tpu as pltpu
from jax.sharding import Mesh
from jax.sharding import PartitionSpec as P

VALUE_DIM = 256
TP = ("tp_0", "tp_1")
FS = ("fs_0", "fs_1")
FS_CORE = ("fs_0", "fs_1", "tp_1")
LINK_SCALE = 32.0


def swap(pieces, axes):
    return lax.all_to_all(pieces, axes, 0, 0, tiled=True)


def to_all(shard, axes):
    size = lax.axis_size(axes)
    return swap(jnp.broadcast_to(shard[None], (size, *shard.shape)), axes)


def in_bf16_parts(values, count):
    parts = []
    for _ in range(count):
        part = lax.reduce_precision(values, 8, 7)
        parts.append(part.astype(jnp.bfloat16))
        values = values - part
    return parts


def raw_kernel(directions, factor, raw, squares):
    values = directions[...].T
    total = None
    for _ in range(3):
        part = values.astype(jnp.bfloat16)
        values = values - part.astype(jnp.float32)
        term = lax.dot_general(
            part, factor[...], (((1,), (1,)), ((), ())), preferred_element_type=jnp.float32
        )
        total = term if total is None else total + term
    raw[...] = total
    width = total.shape[0] // 2
    peers = squares.shape[0]
    for half in range(2):
        own = total[half * width : (half + 1) * width]
        block = jnp.full((peers, 4, 128), jnp.sum(own * own), jnp.float32)
        squares[:, 4 * half : 4 * half + 4, :] = block


def raw_and_squares(directions, factor, peers):
    columns = directions.shape[1]
    return pl.pallas_call(
        raw_kernel,
        out_shape=(
            jax.ShapeDtypeStruct((columns, factor.shape[0]), jnp.float32),
            jax.ShapeDtypeStruct((peers, 8, 128), jnp.float32),
        ),
        name="raw_and_squares",
    )(directions, factor)


def updated(raw, squares, all_masters, masters_here, fs_at, cells):
    columns, rows = raw.shape
    width = columns // 2
    fs_rows = masters_here.shape[1]

    def kernel(at, raw, squares, all_masters, masters_here, key_new, value_new, key_copy, value_copy):
        sums = jnp.sum(squares[...], axis=0)
        start = pl.multiple_of(at[0] * fs_rows, fs_rows)
        for half, (new, copy) in enumerate(((key_new, key_copy), (value_new, value_copy))):
            span = slice(half * width, (half + 1) * width)
            scale = 0.02 / jnp.sqrt(sums[4 * half : 4 * half + 1, 0:1] / cells + 0.01)
            copy[...] = (0.998 * all_masters[span, :] - scale * raw[span, :]).astype(jnp.bfloat16)
            new[...] = 0.998 * masters_here[span, :] - scale * raw[span, pl.ds(start, fs_rows)]

    vmem = pl.BlockSpec(memory_space=pltpu.VMEM)
    return pl.pallas_call(
        kernel,
        in_specs=[pl.BlockSpec(memory_space=pltpu.SMEM), vmem, vmem, vmem, vmem],
        out_shape=(
            jax.ShapeDtypeStruct((width, fs_rows), jnp.float32),
            jax.ShapeDtypeStruct((width, fs_rows), jnp.float32),
            jax.ShapeDtypeStruct((width, rows), jnp.bfloat16),
            jax.ShapeDtypeStruct((width, rows), jnp.bfloat16),
        ),
        name="updated",
    )(fs_at.reshape(1), raw, squares, all_masters, masters_here)


def local(
    normed,
    key_cot,
    first_map,
    second_map,
    lambdas,
    factor,
    key_master,
    value_master,
    key_first,
    key_second,
    value_first,
    value_second,
):
    width, tokens = normed.shape
    cores = lax.axis_size("tp_1")
    chips = lax.axis_size("tp_0")
    fs_size = lax.axis_size(FS)
    rank = factor.shape[1]
    rows = factor.shape[0]
    heads = lambdas.shape[0]
    fs_rows = key_master.shape[0]
    fs_at = lax.axis_index(FS)
    half = tokens // cores
    share = half // chips

    rows_here = lax.axis_index(TP) * width + lax.iota(jnp.int32, width)
    owners = rows_here // VALUE_DIM
    picked = (owners[:, None] == lax.iota(jnp.int32, heads)[None, :]).astype(jnp.float32)
    row_lambda = jnp.sum(picked * lambdas[None, :], axis=1)
    features = jnp.stack([normed[:, c * half : (c + 1) * half] for c in range(cores)])
    features = swap(features, "tp_1").reshape(cores * width, half)

    by_token = features.T.reshape(chips, share, cores * width)
    by_token, first_map, second_map = lax.optimization_barrier((by_token, first_map, second_map))
    by_token = swap(by_token, "tp_0")

    value_cot = (
        first_map.astype(jnp.float32) - row_lambda[:, None] * second_map.astype(jnp.float32)
    ).astype(jnp.bfloat16)
    core = lax.axis_index("tp_1")
    stacked = jnp.concatenate([key_cot, value_cot], axis=0)
    kept = lax.dynamic_slice_in_dim(stacked, core * half, half, 1)
    sent = lax.dynamic_slice_in_dim(stacked, (1 - core) * half, half, 1)
    masters_here = jnp.concatenate([key_master.T, value_master.T], axis=0)
    masters = jnp.broadcast_to(masters_here[None], (fs_size, *masters_here.shape))
    masters, sent = lax.optimization_barrier((masters, sent))
    came = lax.ppermute(sent, "tp_1", [(0, 1), (1, 0)])
    cots = jnp.concatenate([jnp.where(core == 0, kept, came), jnp.where(core == 0, came, kept)])
    cots, by_token = lax.optimization_barrier((cots, by_token))
    product = lax.dot_general(
        by_token.transpose(1, 0, 2).reshape(share, rows),
        factor,
        (((1,), (0,)), ((), ())),
        preferred_element_type=jnp.float32,
    )
    masters, product = lax.optimization_barrier((masters, product))
    masters = swap(masters, FS)
    link = (product * LINK_SCALE).astype(jnp.float16)
    link = lax.all_gather(link, "tp_0", axis=0, tiled=True)

    high, low = in_bf16_parts(link.astype(jnp.float32), 2)
    dims = (((0,), (1,)), ((), ()))
    partial = lax.dot_general(high, cots, dims, preferred_element_type=jnp.float32)
    partial = partial + lax.dot_general(low, cots, dims, preferred_element_type=jnp.float32)
    pieces = partial.reshape(fs_size, rank // fs_size, cores, 2 * width)
    pieces = pieces.transpose(0, 2, 1, 3).reshape(fs_size * cores, rank // fs_size, 2 * width)
    masters, pieces = lax.optimization_barrier((masters, pieces))
    norm_scale = 1.0 / (LINK_SCALE * math.sqrt(tokens * fs_size))
    small = jnp.sum(swap(pieces, FS_CORE), axis=0) * norm_scale

    first = jnp.concatenate([key_first, value_first], axis=1)
    second = jnp.concatenate([key_second, value_second], axis=1)
    first_new = 0.8 * first + 0.2 * small
    second_new = 0.9 * second + 0.1 * small * small
    direction = first_new / (jnp.sqrt(second_new) + 1e-06)
    directions = to_all(direction, FS).reshape(rank, 2 * width)

    raw, squares = raw_and_squares(directions, factor, cores * chips)
    squares = swap(squares, TP)
    cells = rows * width * cores * chips
    all_masters = masters.transpose(1, 0, 2).reshape(2 * width, rows)
    key_new, value_new, key_copy, value_copy = updated(
        raw, squares, all_masters, masters_here, fs_at, cells
    )
    return (
        key_new.T,
        value_new.T,
        key_copy.T,
        value_copy.T,
        first_new[:, :width],
        second_new[:, :width],
        first_new[:, width:],
        second_new[:, width:],
    )


def solution(mesh):
    split = Mesh(mesh.devices.reshape(4, 4, 16, 2), ("fs_0", "fs_1", "tp_0", "tp_1"))
    placed = (
        P(TP, FS),
        P(TP, FS),
        P(TP, FS),
        P(TP, FS),
        P(),
        P(),
        P(FS, TP),
        P(FS, TP),
        P(FS, TP),
        P(FS, TP),
        P(FS, TP),
        P(FS, TP),
    )
    return jax.shard_map(
        local,
        mesh=split,
        in_specs=placed,
        out_specs=(
            P(FS, TP),
            P(FS, TP),
            P(None, TP),
            P(None, TP),
            P(FS, TP),
            P(FS, TP),
            P(FS, TP),
            P(FS, TP),
        ),
        check_vma=False,
    )
```

```python
import math

import jax
import jax.numpy as jnp
from jax import lax
from jax.experimental import pallas as pl
from jax.sharding import Mesh
from jax.sharding import PartitionSpec as P

VALUE_DIM = 256
TP = ("tp_0", "tp_1")
FS = ("fs_0", "fs_1")
FS_CORE = ("fs_0", "fs_1", "tp_1")
LINK_SCALE = 32.0


def swap(pieces, axes):
    return lax.all_to_all(pieces, axes, 0, 0, tiled=True)


def to_all(shard, axes):
    size = lax.axis_size(axes)
    return swap(jnp.broadcast_to(shard[None], (size, *shard.shape)), axes)


def in_bf16_parts(values, count):
    parts = []
    for _ in range(count):
        part = lax.reduce_precision(values, 8, 7)
        parts.append(part.astype(jnp.bfloat16))
        values = values - part
    return parts


def squares_kernel(directions, gram, squares):
    values = directions[...]
    seen = jnp.dot(
        gram[...], values, precision=lax.Precision.HIGHEST, preferred_element_type=jnp.float32
    )
    columns = jnp.sum(values * seen, axis=0, keepdims=True)
    is_key = lax.broadcasted_iota(jnp.int32, columns.shape, 1) < columns.shape[1] // 2
    key = jnp.sum(jnp.where(is_key, columns, 0.0))
    value = jnp.sum(jnp.where(is_key, 0.0, columns))
    squares[...] = jnp.broadcast_to(jnp.where(is_key, key, value)[None], squares.shape)


def squares_of(directions, gram, peers):
    return pl.pallas_call(
        squares_kernel,
        out_shape=jax.ShapeDtypeStruct((peers, 1, directions.shape[1]), jnp.float32),
        name="squares",
    )(directions, gram)


def local(
    normed,
    key_cot,
    first_map,
    second_map,
    lambdas,
    factor,
    key_master,
    value_master,
    key_first,
    key_second,
    value_first,
    value_second,
):
    width, tokens = normed.shape
    cores = lax.axis_size("tp_1")
    chips = lax.axis_size("tp_0")
    fs_size = lax.axis_size(FS)
    rank = factor.shape[1]
    rows = factor.shape[0]
    heads = lambdas.shape[0]
    fs_rows = key_master.shape[0]
    half = tokens // cores
    share = half // chips

    rows_here = lax.axis_index(TP) * width + lax.iota(jnp.int32, width)
    owners = rows_here // VALUE_DIM
    picked = (owners[:, None] == lax.iota(jnp.int32, heads)[None, :]).astype(jnp.float32)
    row_lambda = jnp.sum(picked * lambdas[None, :], axis=1)
    features = jnp.stack([normed[:, c * half : (c + 1) * half] for c in range(cores)])
    features = swap(features, "tp_1").reshape(cores * width, half)

    by_token = features.T.reshape(chips, share, cores * width)
    by_token, first_map, second_map = lax.optimization_barrier((by_token, first_map, second_map))
    by_token = swap(by_token, "tp_0")

    value_cot = (
        first_map.astype(jnp.float32) - row_lambda[:, None] * second_map.astype(jnp.float32)
    ).astype(jnp.bfloat16)
    core = lax.axis_index("tp_1")
    stacked = jnp.concatenate([key_cot, value_cot], axis=0)
    kept = lax.dynamic_slice_in_dim(stacked, core * half, half, 1)
    sent = lax.dynamic_slice_in_dim(stacked, (1 - core) * half, half, 1)
    masters_here = jnp.concatenate([key_master.T, value_master.T], axis=0)
    masters = jnp.broadcast_to(masters_here[None], (fs_size, *masters_here.shape))
    gram = lax.dot_general(
        factor, factor, (((0,), (0,)), ((), ())), preferred_element_type=jnp.float32
    )
    fs_at = lax.axis_index(FS) * fs_rows
    masters, gram, fs_at, sent = lax.optimization_barrier((masters, gram, fs_at, sent))
    came = lax.ppermute(sent, "tp_1", [(0, 1), (1, 0)])
    cots = jnp.concatenate([jnp.where(core == 0, kept, came), jnp.where(core == 0, came, kept)])
    cots, by_token = lax.optimization_barrier((cots, by_token))
    product = lax.dot_general(
        by_token.transpose(1, 0, 2).reshape(share, rows),
        factor,
        (((1,), (0,)), ((), ())),
        preferred_element_type=jnp.float32,
    )
    masters, product = lax.optimization_barrier((masters, product))
    masters = swap(masters, FS)
    link = (product * LINK_SCALE).astype(jnp.float16)
    link = lax.all_gather(link, "tp_0", axis=0, tiled=True)

    high, low = in_bf16_parts(link.astype(jnp.float32), 2)
    dims = (((0,), (1,)), ((), ()))
    partial = lax.dot_general(high, cots, dims, preferred_element_type=jnp.float32)
    partial = partial + lax.dot_general(low, cots, dims, preferred_element_type=jnp.float32)
    pieces = partial.reshape(fs_size, rank // fs_size, cores, 2 * width)
    pieces = pieces.transpose(0, 2, 1, 3).reshape(fs_size * cores, rank // fs_size, 2 * width)
    masters, pieces = lax.optimization_barrier((masters, pieces))
    norm_scale = 1.0 / (LINK_SCALE * math.sqrt(tokens * fs_size))
    small = jnp.sum(swap(pieces, FS_CORE), axis=0) * norm_scale

    first = jnp.concatenate([key_first, value_first], axis=1)
    second = jnp.concatenate([key_second, value_second], axis=1)
    first_new = 0.8 * first + 0.2 * small
    second_new = 0.9 * second + 0.1 * small * small
    direction = first_new / (jnp.sqrt(second_new) + 1e-06)
    directions = to_all(direction, FS).reshape(rank, 2 * width)

    squares = squares_of(directions, gram, cores * chips)
    squares = jnp.sum(swap(squares, TP), axis=(0, 1))
    cells = rows * width * cores * chips
    scales = 0.02 / jnp.sqrt(squares / cells + 0.01)

    raw = sum(
        lax.dot_general(part, factor, (((0,), (1,)), ((), ())), preferred_element_type=jnp.float32)
        for part in in_bf16_parts(directions, 3)
    )
    raw_here = lax.dynamic_slice_in_dim(raw, fs_at, fs_rows, 1)
    all_masters = masters.transpose(1, 0, 2).reshape(2 * width, rows)
    key_new = 0.998 * key_master.T - scales[0] * raw_here[:width]
    value_new = 0.998 * value_master.T - scales[width] * raw_here[width:]
    key_copy = 0.998 * all_masters[:width] - scales[0] * raw[:width]
    value_copy = 0.998 * all_masters[width:] - scales[width] * raw[width:]
    return (
        key_new.T,
        value_new.T,
        key_copy.astype(jnp.bfloat16).T,
        value_copy.astype(jnp.bfloat16).T,
        first_new[:, :width],
        second_new[:, :width],
        first_new[:, width:],
        second_new[:, width:],
    )


def solution(mesh):
    split = Mesh(mesh.devices.reshape(4, 4, 16, 2), ("fs_0", "fs_1", "tp_0", "tp_1"))
    placed = (
        P(TP, FS),
        P(TP, FS),
        P(TP, FS),
        P(TP, FS),
        P(),
        P(),
        P(FS, TP),
        P(FS, TP),
        P(FS, TP),
        P(FS, TP),
        P(FS, TP),
        P(FS, TP),
    )
    return jax.shard_map(
        local,
        mesh=split,
        in_specs=placed,
        out_specs=(
            P(FS, TP),
            P(FS, TP),
            P(None, TP),
            P(None, TP),
            P(FS, TP),
            P(FS, TP),
            P(FS, TP),
            P(FS, TP),
        ),
        check_vma=False,
    )
```

```python
import math

import jax
import jax.numpy as jnp
from jax import lax
from jax.experimental.layout import Layout, with_layout_constraint
from jax.sharding import Mesh
from jax.sharding import PartitionSpec as P

VALUE_DIM = 256
TP = ("tp_0", "tp_1")
FS = ("fs_0", "fs_1")
FS_CORE = ("fs_0", "fs_1", "tp_1")
LINK_SCALE = 32.0


def swap(pieces, axes):
    return lax.all_to_all(pieces, axes, 0, 0, tiled=True)


def to_all(shard, axes):
    size = lax.axis_size(axes)
    return swap(jnp.broadcast_to(shard[None], (size, *shard.shape)), axes)


def in_bf16_parts(values, count):
    parts = []
    for _ in range(count):
        part = lax.reduce_precision(values, 8, 7)
        parts.append(part.astype(jnp.bfloat16))
        values = values - part
    return parts


def local(
    normed,
    key_cot,
    first_map,
    second_map,
    lambdas,
    factor,
    key_master,
    value_master,
    key_first,
    key_second,
    value_first,
    value_second,
):
    width, tokens = normed.shape
    cores = lax.axis_size("tp_1")
    chips = lax.axis_size("tp_0")
    fs_size = lax.axis_size(FS)
    rank = factor.shape[1]
    rows = factor.shape[0]
    heads = lambdas.shape[0]
    fs_rows = key_master.shape[0]
    half = tokens // cores
    share = half // chips

    rows_here = lax.axis_index(TP) * width + lax.iota(jnp.int32, width)
    owners = rows_here // VALUE_DIM
    picked = (owners[:, None] == lax.iota(jnp.int32, heads)[None, :]).astype(jnp.float32)
    row_lambda = jnp.sum(picked * lambdas[None, :], axis=1)
    core = lax.axis_index("tp_1")
    kept = lax.dynamic_slice_in_dim(normed, core * half, half, 1)
    sent = lax.dynamic_slice_in_dim(normed, (1 - core) * half, half, 1)
    sent = with_layout_constraint(sent, Layout(major_to_minor=(0, 1)))
    came = lax.ppermute(sent, "tp_1", [(0, 1), (1, 0)])
    came = with_layout_constraint(came, Layout(major_to_minor=(0, 1)))
    features = jnp.concatenate([kept, came], axis=0)

    by_token = features.T.reshape(chips, share, cores * width)
    by_token, first_map, second_map, blocks, key_master, value_master = lax.optimization_barrier(
        (
            by_token,
            first_map,
            second_map,
            factor.reshape(chips, cores, width, rank),
            key_master,
            value_master,
        )
    )
    by_token = swap(by_token, "tp_0")

    value_cot = (
        first_map.astype(jnp.float32) - row_lambda[:, None] * second_map.astype(jnp.float32)
    ).astype(jnp.bfloat16)
    stacked = jnp.concatenate([key_cot, value_cot], axis=0)
    kept = lax.dynamic_slice_in_dim(stacked, core * half, half, 1)
    sent = lax.dynamic_slice_in_dim(stacked, (1 - core) * half, half, 1)
    masters_here = jnp.concatenate([key_master.T, value_master.T], axis=0)
    masters = jnp.broadcast_to(masters_here[None], (fs_size, *masters_here.shape))
    late_factor = blocks.reshape(rows, rank)
    gram = lax.dot_general(
        late_factor, late_factor, (((0,), (0,)), ((), ())), preferred_element_type=jnp.float32
    )
    own_first = jnp.where(core == 0, blocks, blocks[:, ::-1]).reshape(rows, rank)
    fs_at = lax.axis_index(FS) * fs_rows
    masters, gram, own_first, fs_at, sent = lax.optimization_barrier(
        (masters, gram, own_first, fs_at, sent)
    )
    came = lax.ppermute(sent, "tp_1", [(0, 1), (1, 0)])
    cots = jnp.concatenate([jnp.where(core == 0, kept, came), jnp.where(core == 0, came, kept)])
    cots, by_token = lax.optimization_barrier((cots, by_token))
    product = lax.dot_general(
        by_token.transpose(1, 0, 2).reshape(share, rows),
        own_first,
        (((1,), (0,)), ((), ())),
        preferred_element_type=jnp.float32,
    )
    link = (product * LINK_SCALE).astype(jnp.float16)
    masters, link = lax.optimization_barrier((masters, link))
    masters = swap(masters, FS)
    link = lax.all_gather(link, "tp_0", axis=0, tiled=True)

    high, low = in_bf16_parts(link.astype(jnp.float32), 2)
    dims = (((0,), (1,)), ((), ()))
    partial = lax.dot_general(high, cots, dims, preferred_element_type=jnp.float32)
    partial = partial + lax.dot_general(low, cots, dims, preferred_element_type=jnp.float32)
    pieces = partial.reshape(fs_size, rank // fs_size, cores, 2 * width)
    pieces = pieces.transpose(0, 2, 1, 3).reshape(fs_size * cores, rank // fs_size, 2 * width)
    masters, pieces = lax.optimization_barrier((masters, pieces))
    norm_scale = 1.0 / (LINK_SCALE * math.sqrt(tokens * fs_size))
    small = jnp.sum(swap(pieces, FS_CORE), axis=0) * norm_scale

    first = jnp.concatenate([key_first, value_first], axis=1)
    second = jnp.concatenate([key_second, value_second], axis=1)
    first_new = 0.8 * first + 0.2 * small
    second_new = 0.9 * second + 0.1 * small * small
    direction = first_new / (jnp.sqrt(second_new) + 1e-06)
    directions = to_all(direction, FS).reshape(rank, 2 * width)

    seen = jnp.dot(gram, directions, precision=lax.Precision.HIGHEST)
    squares = jnp.sum(directions * seen, axis=0, keepdims=True)
    squares = jnp.broadcast_to(squares[None], (cores * chips, 1, 2 * width))
    directions, squares, masters, first_new, second_new = lax.optimization_barrier(
        (directions, squares, masters, first_new, second_new)
    )
    squares = jnp.sum(swap(squares, TP).reshape(cores * chips, 2, width), axis=(0, 2))
    cells = rows * width * cores * chips
    scales = 0.02 / jnp.sqrt(squares / cells + 0.01)
    row_scale = jnp.repeat(scales, width)[:, None]

    raw = sum(
        lax.dot_general(part, factor, (((0,), (1,)), ((), ())), preferred_element_type=jnp.float32)
        for part in in_bf16_parts(directions, 3)
    )
    raw_here = lax.dynamic_slice_in_dim(raw, fs_at, fs_rows, 1, allow_negative_indices=False)
    all_masters = masters.transpose(1, 0, 2).reshape(2 * width, rows)
    new_here = 0.998 * masters_here - row_scale * raw_here
    copies = (0.998 * all_masters - row_scale * raw).astype(jnp.bfloat16)
    return (
        new_here[:width].T,
        new_here[width:].T,
        copies[:width].T,
        copies[width:].T,
        first_new[:, :width],
        second_new[:, :width],
        first_new[:, width:],
        second_new[:, width:],
    )


def solution(mesh):
    split = Mesh(mesh.devices.reshape(4, 4, 16, 2), ("fs_0", "fs_1", "tp_0", "tp_1"))
    placed = (
        P(TP, FS),
        P(TP, FS),
        P(TP, FS),
        P(TP, FS),
        P(),
        P(),
        P(FS, TP),
        P(FS, TP),
        P(FS, TP),
        P(FS, TP),
        P(FS, TP),
        P(FS, TP),
    )
    return jax.shard_map(
        local,
        mesh=split,
        in_specs=placed,
        out_specs=(
            P(FS, TP),
            P(FS, TP),
            P(None, TP),
            P(None, TP),
            P(FS, TP),
            P(FS, TP),
            P(FS, TP),
            P(FS, TP),
        ),
        check_vma=False,
    )
```

```python
import math

import jax
import jax.numpy as jnp
from jax import lax
from jax.experimental.layout import Layout, with_layout_constraint
from jax.sharding import Mesh
from jax.sharding import PartitionSpec as P

VALUE_DIM = 256
TP = ("tp_0", "tp_1")
FS = ("fs_0", "fs_1")
FS_CORE = ("fs_0", "fs_1", "tp_1")
LINK_SCALE = 32.0


def swap(pieces, axes):
    return lax.all_to_all(pieces, axes, 0, 0, tiled=True)


def to_all(shard, axes):
    size = lax.axis_size(axes)
    return swap(jnp.broadcast_to(shard[None], (size, *shard.shape)), axes)


def in_bf16_parts(values, count):
    parts = []
    for _ in range(count):
        part = lax.reduce_precision(values, 8, 7)
        parts.append(part.astype(jnp.bfloat16))
        values = values - part
    return parts


def local(
    normed,
    key_cot,
    first_map,
    second_map,
    lambdas,
    factor,
    key_master,
    value_master,
    key_first,
    key_second,
    value_first,
    value_second,
):
    width, tokens = normed.shape
    cores = lax.axis_size("tp_1")
    chips = lax.axis_size("tp_0")
    fs_size = lax.axis_size(FS)
    rank = factor.shape[1]
    rows = factor.shape[0]
    heads = lambdas.shape[0]
    fs_rows = key_master.shape[0]
    half = tokens // cores
    share = half // chips

    rows_here = lax.axis_index(TP) * width + lax.iota(jnp.int32, width)
    owners = rows_here // VALUE_DIM
    picked = (owners[:, None] == lax.iota(jnp.int32, heads)[None, :]).astype(jnp.float32)
    row_lambda = jnp.sum(picked * lambdas[None, :], axis=1)
    core = lax.axis_index("tp_1")
    came = lax.ppermute(normed, "tp_1", [(0, 1), (1, 0)])
    came = with_layout_constraint(came, Layout(major_to_minor=(0, 1)))
    kept, came = (
        lax.dynamic_slice_in_dim(side, core * half, half, 1, allow_negative_indices=False)
        for side in (normed, came)
    )
    features = jnp.concatenate([kept, came], axis=0)

    by_token = features.T.reshape(chips, share, cores * width)
    by_token, first_map, second_map, blocks, key_master, value_master = lax.optimization_barrier(
        (
            by_token,
            first_map,
            second_map,
            factor.reshape(chips, cores, width, rank),
            key_master,
            value_master,
        )
    )
    by_token = swap(by_token, "tp_0")

    value_cot = (
        first_map.astype(jnp.float32) - row_lambda[:, None] * second_map.astype(jnp.float32)
    ).astype(jnp.bfloat16)
    stacked = jnp.concatenate([key_cot, value_cot], axis=0)
    kept = lax.dynamic_slice_in_dim(stacked, core * half, half, 1)
    sent = lax.dynamic_slice_in_dim(stacked, (1 - core) * half, half, 1)
    masters_here = jnp.concatenate([key_master.T, value_master.T], axis=0)
    masters = jnp.broadcast_to(masters_here[None], (fs_size, *masters_here.shape))
    late_factor = blocks.reshape(rows, rank)
    gram = lax.dot_general(
        late_factor, late_factor, (((0,), (0,)), ((), ())), preferred_element_type=jnp.float32
    )
    own_first = jnp.where(core == 0, blocks, blocks[:, ::-1]).reshape(rows, rank)
    fs_at = lax.axis_index(FS) * fs_rows
    masters, gram, own_first, fs_at, sent = lax.optimization_barrier(
        (masters, gram, own_first, fs_at, sent)
    )
    came = lax.ppermute(sent, "tp_1", [(0, 1), (1, 0)])
    cots = jnp.concatenate([jnp.where(core == 0, kept, came), jnp.where(core == 0, came, kept)])
    cots, masters, by_token = lax.optimization_barrier((cots, masters, by_token))
    product = lax.dot_general(
        by_token.transpose(1, 0, 2).reshape(share, rows),
        own_first,
        (((1,), (0,)), ((), ())),
        preferred_element_type=jnp.float32,
    )
    link = (product * LINK_SCALE).astype(jnp.float16)
    masters = swap(masters, FS)
    link = lax.all_gather(link, "tp_0", axis=0, tiled=True)

    high, low = in_bf16_parts(link.astype(jnp.float32), 2)
    dims = (((0,), (1,)), ((), ()))
    partial = lax.dot_general(high, cots, dims, preferred_element_type=jnp.float32)
    partial = partial + lax.dot_general(low, cots, dims, preferred_element_type=jnp.float32)
    pieces = partial.reshape(fs_size, rank // fs_size, cores, 2 * width)
    pieces = pieces.transpose(0, 2, 1, 3).reshape(fs_size * cores, rank // fs_size, 2 * width)
    masters, pieces = lax.optimization_barrier((masters, pieces))
    norm_scale = 1.0 / (LINK_SCALE * math.sqrt(tokens * fs_size))
    small = jnp.sum(swap(pieces, FS_CORE), axis=0) * norm_scale

    first = jnp.concatenate([key_first, value_first], axis=1)
    second = jnp.concatenate([key_second, value_second], axis=1)
    first_new = 0.8 * first + 0.2 * small
    second_new = 0.9 * second + 0.1 * small * small
    direction = first_new / (jnp.sqrt(second_new) + 1e-06)
    directions = to_all(direction, FS).reshape(rank, 2 * width)

    seen = jnp.dot(gram, directions, precision=lax.Precision.HIGHEST)
    squares = jnp.sum(directions * seen, axis=0, keepdims=True)
    squares = jnp.broadcast_to(squares[None], (cores * chips, 1, 2 * width))
    directions, squares, masters, first_new, second_new = lax.optimization_barrier(
        (directions, squares, masters, first_new, second_new)
    )
    squares = jnp.sum(swap(squares, TP).reshape(cores * chips, 2, width), axis=(0, 2))
    cells = rows * width * cores * chips
    scales = 0.02 / jnp.sqrt(squares / cells + 0.01)

    raw = sum(
        lax.dot_general(part, factor, (((0,), (1,)), ((), ())), preferred_element_type=jnp.float32)
        for part in in_bf16_parts(directions, 3)
    )
    raw_here = lax.dynamic_slice_in_dim(raw, fs_at, fs_rows, 1, allow_negative_indices=False)
    all_masters = masters.transpose(1, 0, 2).reshape(2 * width, rows)
    raw, raw_here, all_masters = lax.optimization_barrier((raw, raw_here, all_masters))
    row_scale = lax.optimization_barrier(jnp.repeat(scales, width)[:, None])
    new, copies = [], []
    for at in (0, width):
        span = slice(at, at + width)
        scale = row_scale[span]
        new.append((0.998 * masters_here[span] - scale * raw_here[span]).T)
        copies.append((0.998 * all_masters[span] - scale * raw[span]).astype(jnp.bfloat16).T)
    return (
        *new,
        *copies,
        first_new[:, :width],
        second_new[:, :width],
        first_new[:, width:],
        second_new[:, width:],
    )


def solution(mesh):
    split = Mesh(mesh.devices.reshape(4, 4, 16, 2), ("fs_0", "fs_1", "tp_0", "tp_1"))
    placed = (
        P(TP, FS),
        P(TP, FS),
        P(TP, FS),
        P(TP, FS),
        P(),
        P(),
        P(FS, TP),
        P(FS, TP),
        P(FS, TP),
        P(FS, TP),
        P(FS, TP),
        P(FS, TP),
    )
    return jax.shard_map(
        local,
        mesh=split,
        in_specs=placed,
        out_specs=(
            P(FS, TP),
            P(FS, TP),
            P(None, TP),
            P(None, TP),
            P(FS, TP),
            P(FS, TP),
            P(FS, TP),
            P(FS, TP),
        ),
        check_vma=False,
    )
```

```python
import math

import jax
import jax.numpy as jnp
from jax import lax
from jax.experimental.layout import Layout, with_layout_constraint
from jax.sharding import Mesh
from jax.sharding import PartitionSpec as P

VALUE_DIM = 256
TP = ("tp_0", "tp_1")
FS = ("fs_0", "fs_1")
FS_CORE = ("fs_0", "fs_1", "tp_1")
LINK_SCALE = 32.0
MASTER_SCALE = 1024.0


def swap(pieces, axes):
    return lax.all_to_all(pieces, axes, 0, 0, tiled=True)


def to_all(shard, axes):
    size = lax.axis_size(axes)
    return swap(jnp.broadcast_to(shard[None], (size, *shard.shape)), axes)


def in_bf16_parts(values, count):
    parts = []
    for _ in range(count):
        part = lax.reduce_precision(values, 8, 7)
        parts.append(part.astype(jnp.bfloat16))
        values = values - part
    return parts


def coded(masters):
    return (masters * jnp.abs(masters) * MASTER_SCALE**2).astype(jnp.float16)


def decoded(codes):
    values = codes.astype(jnp.float32)
    return jnp.sign(values) * jnp.sqrt(jnp.abs(values)) * (1.0 / MASTER_SCALE)


def local(
    normed,
    key_cot,
    first_map,
    second_map,
    lambdas,
    factor,
    key_master,
    value_master,
    key_first,
    key_second,
    value_first,
    value_second,
):
    width, tokens = normed.shape
    cores = lax.axis_size("tp_1")
    chips = lax.axis_size("tp_0")
    fs_size = lax.axis_size(FS)
    rank = factor.shape[1]
    rows = factor.shape[0]
    heads = lambdas.shape[0]
    fs_rows = key_master.shape[0]
    half = tokens // cores
    share = half // chips

    rows_here = lax.axis_index(TP) * width + lax.iota(jnp.int32, width)
    owners = rows_here // VALUE_DIM
    picked = (owners[:, None] == lax.iota(jnp.int32, heads)[None, :]).astype(jnp.float32)
    row_lambda = jnp.sum(picked * lambdas[None, :], axis=1)
    core = lax.axis_index("tp_1")
    came = lax.ppermute(normed, "tp_1", [(0, 1), (1, 0)])
    came = with_layout_constraint(came, Layout(major_to_minor=(0, 1)))
    kept, came = (
        lax.dynamic_slice_in_dim(side, core * half, half, 1, allow_negative_indices=False)
        for side in (normed, came)
    )
    features = jnp.concatenate([kept, came], axis=0)

    by_token = features.T.reshape(chips, share, cores * width)
    by_token, first_map, second_map, blocks, key_master, value_master = lax.optimization_barrier(
        (
            by_token,
            first_map,
            second_map,
            factor.reshape(chips, cores, width, rank),
            key_master,
            value_master,
        )
    )
    by_token = swap(by_token, "tp_0")

    value_cot = (
        first_map.astype(jnp.float32) - row_lambda[:, None] * second_map.astype(jnp.float32)
    ).astype(jnp.bfloat16)
    stacked = jnp.concatenate([key_cot, value_cot], axis=0)
    kept = lax.dynamic_slice_in_dim(stacked, core * half, half, 1)
    sent = lax.dynamic_slice_in_dim(stacked, (1 - core) * half, half, 1)
    masters_here = jnp.concatenate([key_master.T, value_master.T], axis=0)
    masters = coded(masters_here)
    masters = jnp.broadcast_to(masters[None], (fs_size, *masters.shape))
    late_factor = blocks.reshape(rows, rank)
    gram = lax.dot_general(
        late_factor, late_factor, (((0,), (0,)), ((), ())), preferred_element_type=jnp.float32
    )
    own_first = jnp.where(core == 0, blocks, blocks[:, ::-1]).reshape(rows, rank)
    fs_at = lax.axis_index(FS) * fs_rows
    masters, gram, own_first, fs_at, sent = lax.optimization_barrier(
        (masters, gram, own_first, fs_at, sent)
    )
    came = lax.ppermute(sent, "tp_1", [(0, 1), (1, 0)])
    cots = jnp.concatenate([jnp.where(core == 0, kept, came), jnp.where(core == 0, came, kept)])
    cots, masters, by_token = lax.optimization_barrier((cots, masters, by_token))
    product = lax.dot_general(
        by_token.transpose(1, 0, 2).reshape(share, rows),
        own_first,
        (((1,), (0,)), ((), ())),
        preferred_element_type=jnp.float32,
    )
    link = (product * LINK_SCALE).astype(jnp.float16)
    masters = swap(masters, FS)
    link = lax.all_gather(link, "tp_0", axis=0, tiled=True)

    high, low = in_bf16_parts(link.astype(jnp.float32), 2)
    dims = (((0,), (1,)), ((), ()))
    partial = lax.dot_general(high, cots, dims, preferred_element_type=jnp.float32)
    partial = partial + lax.dot_general(low, cots, dims, preferred_element_type=jnp.float32)
    pieces = partial.reshape(fs_size, rank // fs_size, cores, 2 * width)
    pieces = pieces.transpose(0, 2, 1, 3).reshape(fs_size * cores, rank // fs_size, 2 * width)
    masters, pieces = lax.optimization_barrier((masters, pieces))
    norm_scale = 1.0 / (LINK_SCALE * math.sqrt(tokens * fs_size))
    small = jnp.sum(swap(pieces, FS_CORE), axis=0) * norm_scale

    first = jnp.concatenate([key_first, value_first], axis=1)
    second = jnp.concatenate([key_second, value_second], axis=1)
    first_new = 0.8 * first + 0.2 * small
    second_new = 0.9 * second + 0.1 * small * small
    direction = first_new / (jnp.sqrt(second_new) + 1e-06)
    directions = to_all(direction, FS).reshape(rank, 2 * width)

    seen = jnp.dot(gram, directions, precision=lax.Precision.HIGHEST)
    squares = jnp.sum(directions * seen, axis=0, keepdims=True)
    squares = jnp.broadcast_to(squares[None], (cores * chips, 1, 2 * width))
    directions, squares, masters, first_new, second_new = lax.optimization_barrier(
        (directions, squares, masters, first_new, second_new)
    )
    squares = jnp.sum(swap(squares, TP).reshape(cores * chips, 2, width), axis=(0, 2))
    cells = rows * width * cores * chips
    scales = 0.02 / jnp.sqrt(squares / cells + 0.01)

    raw = sum(
        lax.dot_general(part, factor, (((0,), (1,)), ((), ())), preferred_element_type=jnp.float32)
        for part in in_bf16_parts(directions, 3)
    )
    raw_here = lax.dynamic_slice_in_dim(raw, fs_at, fs_rows, 1, allow_negative_indices=False)
    all_masters = decoded(masters).transpose(1, 0, 2).reshape(2 * width, rows)
    raw, raw_here, all_masters = lax.optimization_barrier((raw, raw_here, all_masters))
    row_scale = lax.optimization_barrier(jnp.repeat(scales, width)[:, None])
    new, copies = [], []
    for at in (0, width):
        span = slice(at, at + width)
        scale = row_scale[span]
        new.append((0.998 * masters_here[span] - scale * raw_here[span]).T)
        copies.append((0.998 * all_masters[span] - scale * raw[span]).astype(jnp.bfloat16).T)
    return (
        *new,
        *copies,
        first_new[:, :width],
        second_new[:, :width],
        first_new[:, width:],
        second_new[:, width:],
    )


def solution(mesh):
    split = Mesh(mesh.devices.reshape(4, 4, 16, 2), ("fs_0", "fs_1", "tp_0", "tp_1"))
    placed = (
        P(TP, FS),
        P(TP, FS),
        P(TP, FS),
        P(TP, FS),
        P(),
        P(),
        P(FS, TP),
        P(FS, TP),
        P(FS, TP),
        P(FS, TP),
        P(FS, TP),
        P(FS, TP),
    )
    return jax.shard_map(
        local,
        mesh=split,
        in_specs=placed,
        out_specs=(
            P(FS, TP),
            P(FS, TP),
            P(None, TP),
            P(None, TP),
            P(FS, TP),
            P(FS, TP),
            P(FS, TP),
            P(FS, TP),
        ),
        check_vma=False,
    )
```

```python
import math

import jax
import jax.numpy as jnp
from jax import lax
from jax.experimental.layout import Layout, with_layout_constraint
from jax.sharding import Mesh
from jax.sharding import PartitionSpec as P

VALUE_DIM = 256
TP = ("tp_0", "tp_1")
FS = ("fs_0", "fs_1")
FS_CORE = ("fs_0", "fs_1", "tp_1")
LINK_SCALE = 32.0
FIRST_CHIP = 11
FIRST_CORE = 1


def swap(pieces, axes, groups=None):
    return lax.all_to_all(pieces, axes, 0, 0, tiled=True, axis_index_groups=groups)


def to_all(shard, axes):
    size = lax.axis_size(axes)
    return swap(jnp.broadcast_to(shard[None], (size, *shard.shape)), axes)


def core_order(cores):
    return [(FIRST_CORE + c) % cores for c in range(cores)]


def chip_order(chips):
    return [(FIRST_CHIP + z) % chips for z in range(chips)]


def in_bf16_parts(values, count):
    parts = []
    for _ in range(count):
        part = lax.reduce_precision(values, 8, 7)
        parts.append(part.astype(jnp.bfloat16))
        values = values - part
    return parts


def local(
    normed,
    key_cot,
    first_map,
    second_map,
    lambdas,
    factor,
    key_master,
    value_master,
    key_first,
    key_second,
    value_first,
    value_second,
):
    width, tokens = normed.shape
    cores = lax.axis_size("tp_1")
    chips = lax.axis_size("tp_0")
    fs_size = lax.axis_size(FS)
    rank = factor.shape[1]
    rows = factor.shape[0]
    heads = lambdas.shape[0]
    fs_rows = key_master.shape[0]
    half = tokens // cores
    rings = [[z * cores + c for z in chip_order(chips)] for c in range(cores)]
    whole = [[z * cores + c for z in chip_order(chips) for c in core_order(cores)]]
    planes = [[f * cores + c for f in range(fs_size) for c in core_order(cores)]]
    share = half // chips

    rows_here = lax.axis_index(TP) * width + lax.iota(jnp.int32, width)
    owners = rows_here // VALUE_DIM
    picked = (owners[:, None] == lax.iota(jnp.int32, heads)[None, :]).astype(jnp.float32)
    row_lambda = jnp.sum(picked * lambdas[None, :], axis=1)
    core = lax.axis_index("tp_1")
    came = lax.ppermute(normed, "tp_1", [(0, 1), (1, 0)])
    came = with_layout_constraint(came, Layout(major_to_minor=(0, 1)))
    kept, came = (
        lax.dynamic_slice_in_dim(side, core * half, half, 1, allow_negative_indices=False)
        for side in (normed, came)
    )
    features = jnp.concatenate([kept, came], axis=0)

    by_token = features.T.reshape(chips, share, cores * width)
    by_token, first_map, second_map, blocks, key_master, value_master = lax.optimization_barrier(
        (
            by_token,
            first_map,
            second_map,
            factor.reshape(chips, cores, width, rank),
            key_master,
            value_master,
        )
    )
    by_token = swap(by_token, TP, rings)

    value_cot = (
        first_map.astype(jnp.float32) - row_lambda[:, None] * second_map.astype(jnp.float32)
    ).astype(jnp.bfloat16)
    stacked = jnp.concatenate([key_cot, value_cot], axis=0)
    kept = lax.dynamic_slice_in_dim(stacked, core * half, half, 1)
    sent = lax.dynamic_slice_in_dim(stacked, (1 - core) * half, half, 1)
    masters_here = jnp.concatenate([key_master.T, value_master.T], axis=0)
    masters = jnp.broadcast_to(masters_here[None], (fs_size, *masters_here.shape))
    late_factor = blocks.reshape(rows, rank)
    gram = lax.dot_general(
        late_factor, late_factor, (((0,), (0,)), ((), ())), preferred_element_type=jnp.float32
    )
    own_first = jnp.where(core == 0, blocks, blocks[:, ::-1])
    own_first = jnp.roll(own_first, -FIRST_CHIP, axis=0).reshape(rows, rank)
    fs_at = lax.axis_index(FS) * fs_rows
    masters, gram, own_first, fs_at, sent = lax.optimization_barrier(
        (masters, gram, own_first, fs_at, sent)
    )
    came = lax.ppermute(sent, "tp_1", [(0, 1), (1, 0)])
    is_first = core == FIRST_CORE
    cots = jnp.concatenate([jnp.where(is_first, kept, came), jnp.where(is_first, came, kept)])
    cots, masters, by_token = lax.optimization_barrier((cots, masters, by_token))
    product = lax.dot_general(
        by_token.transpose(1, 0, 2).reshape(share, rows),
        own_first,
        (((1,), (0,)), ((), ())),
        preferred_element_type=jnp.float32,
    )
    link = (product * LINK_SCALE).astype(jnp.float16)
    masters = swap(masters, FS)
    link = lax.all_gather(link, TP, axis=0, tiled=True, axis_index_groups=rings)

    high, low = in_bf16_parts(link.astype(jnp.float32), 2)
    dims = (((0,), (1,)), ((), ()))
    partial = lax.dot_general(high, cots, dims, preferred_element_type=jnp.float32)
    partial = partial + lax.dot_general(low, cots, dims, preferred_element_type=jnp.float32)
    pieces = partial.reshape(fs_size, rank // fs_size, cores, 2 * width)
    pieces = pieces.transpose(0, 2, 1, 3).reshape(fs_size * cores, rank // fs_size, 2 * width)
    masters, pieces = lax.optimization_barrier((masters, pieces))
    norm_scale = 1.0 / (LINK_SCALE * math.sqrt(tokens * fs_size))
    small = jnp.sum(swap(pieces, FS_CORE, planes), axis=0) * norm_scale

    first = jnp.concatenate([key_first, value_first], axis=1)
    second = jnp.concatenate([key_second, value_second], axis=1)
    first_new = 0.8 * first + 0.2 * small
    second_new = 0.9 * second + 0.1 * small * small
    direction = first_new / (jnp.sqrt(second_new) + 1e-06)
    directions = to_all(direction, FS).reshape(rank, 2 * width)

    seen = jnp.dot(gram, directions, precision=lax.Precision.HIGHEST)
    squares = jnp.sum(directions * seen, axis=0, keepdims=True)
    squares = jnp.broadcast_to(squares[None], (cores * chips, 1, 2 * width))
    directions, squares, masters, first_new, second_new = lax.optimization_barrier(
        (directions, squares, masters, first_new, second_new)
    )
    squares = swap(squares, TP, whole)
    raw = sum(
        lax.dot_general(part, factor, (((0,), (1,)), ((), ())), preferred_element_type=jnp.float32)
        for part in in_bf16_parts(directions, 3)
    )
    raw_here = lax.dynamic_slice_in_dim(raw, fs_at, fs_rows, 1, allow_negative_indices=False)
    all_masters = masters.transpose(1, 0, 2).reshape(2 * width, rows)
    squares = jnp.sum(squares.reshape(cores * chips, 2, width), axis=(0, 2))
    cells = rows * width * cores * chips
    scales = 0.02 / jnp.sqrt(squares / cells + 0.01)

    raw, raw_here, all_masters = lax.optimization_barrier((raw, raw_here, all_masters))
    row_scale = lax.optimization_barrier(jnp.repeat(scales, width)[:, None])
    new, copies = [], []
    for at in (0, width):
        span = slice(at, at + width)
        scale = row_scale[span]
        new.append((0.998 * masters_here[span] - scale * raw_here[span]).T)
        copies.append((0.998 * all_masters[span] - scale * raw[span]).astype(jnp.bfloat16).T)
    return (
        *new,
        *copies,
        first_new[:, :width],
        second_new[:, :width],
        first_new[:, width:],
        second_new[:, width:],
    )


def solution(mesh):
    split = Mesh(mesh.devices.reshape(4, 4, 16, 2), ("fs_0", "fs_1", "tp_0", "tp_1"))
    placed = (
        P(TP, FS),
        P(TP, FS),
        P(TP, FS),
        P(TP, FS),
        P(),
        P(),
        P(FS, TP),
        P(FS, TP),
        P(FS, TP),
        P(FS, TP),
        P(FS, TP),
        P(FS, TP),
    )
    return jax.shard_map(
        local,
        mesh=split,
        in_specs=placed,
        out_specs=(
            P(FS, TP),
            P(FS, TP),
            P(None, TP),
            P(None, TP),
            P(FS, TP),
            P(FS, TP),
            P(FS, TP),
            P(FS, TP),
        ),
        check_vma=False,
    )
```

```python
import math

import jax
import jax.numpy as jnp
from jax import lax
from jax.experimental.layout import Layout, with_layout_constraint
from jax.sharding import Mesh
from jax.sharding import PartitionSpec as P

VALUE_DIM = 256
TP = ("tp_0", "tp_1")
FS = ("fs_0", "fs_1")
FS_CORE = ("fs_0", "fs_1", "tp_1")
LINK_SCALE = 32.0
FIRST_CHIP = 11
FIRST_CORE = 1
FIRST_PLANE = 10


def swap(pieces, axes, groups=None):
    return lax.all_to_all(pieces, axes, 0, 0, tiled=True, axis_index_groups=groups)


def to_all(shard, axes, groups):
    size = lax.axis_size(axes)
    return swap(jnp.broadcast_to(shard[None], (size, *shard.shape)), axes, groups)


def core_order(cores):
    return [(FIRST_CORE + c) % cores for c in range(cores)]


def chip_order(chips):
    return [(FIRST_CHIP + z) % chips for z in range(chips)]


def in_bf16_parts(values, count):
    parts = []
    for _ in range(count):
        part = lax.reduce_precision(values, 8, 7)
        parts.append(part.astype(jnp.bfloat16))
        values = values - part
    return parts


def local(
    normed,
    key_cot,
    first_map,
    second_map,
    lambdas,
    factor,
    key_master,
    value_master,
    key_first,
    key_second,
    value_first,
    value_second,
):
    width, tokens = normed.shape
    cores = lax.axis_size("tp_1")
    chips = lax.axis_size("tp_0")
    fs_size = lax.axis_size(FS)
    rank = factor.shape[1]
    rows = factor.shape[0]
    heads = lambdas.shape[0]
    fs_rows = key_master.shape[0]
    half = tokens // cores
    rings = [[z * cores + c for z in chip_order(chips)] for c in range(cores)]
    whole = [[z * cores + c for z in chip_order(chips) for c in core_order(cores)]]
    order = [(FIRST_PLANE + f) % fs_size for f in range(fs_size)]
    planes = [[f * cores + c for f in order for c in core_order(cores)]]
    share = half // chips

    rows_here = lax.axis_index(TP) * width + lax.iota(jnp.int32, width)
    owners = rows_here // VALUE_DIM
    picked = (owners[:, None] == lax.iota(jnp.int32, heads)[None, :]).astype(jnp.float32)
    row_lambda = jnp.sum(picked * lambdas[None, :], axis=1)
    core = lax.axis_index("tp_1")
    came = lax.ppermute(normed, "tp_1", [(0, 1), (1, 0)])
    came = with_layout_constraint(came, Layout(major_to_minor=(0, 1)))
    kept, came = (
        lax.dynamic_slice_in_dim(side, core * half, half, 1, allow_negative_indices=False)
        for side in (normed, came)
    )
    features = jnp.concatenate([kept, came], axis=0)

    by_token = features.T.reshape(chips, share, cores * width)
    by_token, first_map, second_map, factor, key_master, value_master = lax.optimization_barrier(
        (
            by_token,
            first_map,
            second_map,
            factor,
            key_master,
            value_master,
        )
    )
    by_token = swap(by_token, TP, rings)

    value_cot = (
        first_map.astype(jnp.float32) - row_lambda[:, None] * second_map.astype(jnp.float32)
    ).astype(jnp.bfloat16)
    stacked = jnp.concatenate([key_cot, value_cot], axis=0)
    kept = lax.dynamic_slice_in_dim(stacked, core * half, half, 1)
    sent = lax.dynamic_slice_in_dim(stacked, (1 - core) * half, half, 1)
    masters_here = jnp.concatenate([key_master.T, value_master.T], axis=0)
    masters = jnp.broadcast_to(masters_here[None], (fs_size, *masters_here.shape))
    factor = jnp.roll(factor, -FIRST_PLANE * (rank // fs_size), axis=1)
    gram = lax.dot_general(
        factor, factor, (((0,), (0,)), ((), ())), preferred_element_type=jnp.float32
    )
    blocks = factor.reshape(chips, cores, width, rank)
    own_first = jnp.where(core == 0, blocks, blocks[:, ::-1])
    own_first = jnp.roll(own_first, -FIRST_CHIP, axis=0).reshape(rows, rank)
    fs_at = lax.axis_index(FS) * fs_rows
    masters, gram, own_first, fs_at, sent = lax.optimization_barrier(
        (masters, gram, own_first, fs_at, sent)
    )
    came = lax.ppermute(sent, "tp_1", [(0, 1), (1, 0)])
    is_first = core == FIRST_CORE
    cots = jnp.concatenate([jnp.where(is_first, kept, came), jnp.where(is_first, came, kept)])
    cots, masters, by_token = lax.optimization_barrier((cots, masters, by_token))
    product = lax.dot_general(
        by_token.transpose(1, 0, 2).reshape(share, rows),
        own_first,
        (((1,), (0,)), ((), ())),
        preferred_element_type=jnp.float32,
    )
    link = (product * LINK_SCALE).astype(jnp.float16)
    masters = swap(masters, FS, [order])
    link = lax.all_gather(link, TP, axis=0, tiled=True, axis_index_groups=rings)

    high, low = in_bf16_parts(link.astype(jnp.float32), 2)
    dims = (((0,), (1,)), ((), ()))
    partial = lax.dot_general(high, cots, dims, preferred_element_type=jnp.float32)
    partial = partial + lax.dot_general(low, cots, dims, preferred_element_type=jnp.float32)
    pieces = partial.reshape(fs_size, rank // fs_size, cores, 2 * width)
    pieces = pieces.transpose(0, 2, 1, 3).reshape(fs_size * cores, rank // fs_size, 2 * width)
    masters, pieces = lax.optimization_barrier((masters, pieces))
    norm_scale = 1.0 / (LINK_SCALE * math.sqrt(tokens * fs_size))
    small = jnp.sum(swap(pieces, FS_CORE, planes), axis=0) * norm_scale

    first = jnp.concatenate([key_first, value_first], axis=1)
    second = jnp.concatenate([key_second, value_second], axis=1)
    first_new = 0.8 * first + 0.2 * small
    second_new = 0.9 * second + 0.1 * small * small
    direction = first_new / (jnp.sqrt(second_new) + 1e-06)
    directions = to_all(direction, FS, [order]).reshape(rank, 2 * width)

    seen = jnp.dot(gram, directions, precision=lax.Precision.HIGHEST)
    squares = jnp.sum(directions * seen, axis=0, keepdims=True)
    squares = jnp.broadcast_to(squares[None], (cores * chips, 1, 2 * width))
    directions, squares, masters, first_new, second_new = lax.optimization_barrier(
        (directions, squares, masters, first_new, second_new)
    )
    squares = swap(squares, TP, whole)
    raw = sum(
        lax.dot_general(part, factor, (((0,), (1,)), ((), ())), preferred_element_type=jnp.float32)
        for part in in_bf16_parts(directions, 3)
    )
    raw_here = lax.dynamic_slice_in_dim(raw, fs_at, fs_rows, 1, allow_negative_indices=False)
    all_masters = jnp.roll(masters, FIRST_PLANE, axis=0).transpose(1, 0, 2).reshape(2 * width, rows)
    squares = jnp.sum(squares.reshape(cores * chips, 2, width), axis=(0, 2))
    cells = rows * width * cores * chips
    scales = 0.02 / jnp.sqrt(squares / cells + 0.01)

    raw, raw_here, all_masters = lax.optimization_barrier((raw, raw_here, all_masters))
    row_scale = lax.optimization_barrier(jnp.repeat(scales, width)[:, None])
    new, copies = [], []
    for at in (0, width):
        span = slice(at, at + width)
        scale = row_scale[span]
        new.append((0.998 * masters_here[span] - scale * raw_here[span]).T)
        copies.append((0.998 * all_masters[span] - scale * raw[span]).astype(jnp.bfloat16).T)
    return (
        *new,
        *copies,
        first_new[:, :width],
        second_new[:, :width],
        first_new[:, width:],
        second_new[:, width:],
    )


def solution(mesh):
    split = Mesh(mesh.devices.reshape(4, 4, 16, 2), ("fs_0", "fs_1", "tp_0", "tp_1"))
    placed = (
        P(TP, FS),
        P(TP, FS),
        P(TP, FS),
        P(TP, FS),
        P(),
        P(),
        P(FS, TP),
        P(FS, TP),
        P(FS, TP),
        P(FS, TP),
        P(FS, TP),
        P(FS, TP),
    )
    return jax.shard_map(
        local,
        mesh=split,
        in_specs=placed,
        out_specs=(
            P(FS, TP),
            P(FS, TP),
            P(None, TP),
            P(None, TP),
            P(FS, TP),
            P(FS, TP),
            P(FS, TP),
            P(FS, TP),
        ),
        check_vma=False,
    )
```

```python
import math

import jax
import jax.numpy as jnp
from jax import lax
from jax.experimental.layout import Layout, with_layout_constraint
from jax.sharding import Mesh
from jax.sharding import PartitionSpec as P

VALUE_DIM = 256
TP = ("tp_0", "tp_1")
FS = ("fs_0", "fs_1")
FS_CORE = ("fs_0", "fs_1", "tp_1")
LINK_SCALE = 32.0
FIRST_CHIP = 12
GATHER_CHIP = 0
FIRST_CORE = 1
FIRST_PLANE = 10


def swap(pieces, axes, groups=None):
    return lax.all_to_all(pieces, axes, 0, 0, tiled=True, axis_index_groups=groups)


def to_all(shard, axes, groups):
    size = lax.axis_size(axes)
    return swap(jnp.broadcast_to(shard[None], (size, *shard.shape)), axes, groups)


def core_order(cores):
    return [(FIRST_CORE + c) % cores for c in range(cores)]


def rings_from(first, chips, cores):
    return [[(first + z) % chips * cores + c for z in range(chips)] for c in range(cores)]


def in_bf16_parts(values, count):
    parts = []
    for _ in range(count):
        part = lax.reduce_precision(values, 8, 7)
        parts.append(part.astype(jnp.bfloat16))
        values = values - part
    return parts


def local(
    normed,
    key_cot,
    first_map,
    second_map,
    lambdas,
    factor,
    key_master,
    value_master,
    key_first,
    key_second,
    value_first,
    value_second,
):
    width, tokens = normed.shape
    cores = lax.axis_size("tp_1")
    chips = lax.axis_size("tp_0")
    fs_size = lax.axis_size(FS)
    rank = factor.shape[1]
    rows = factor.shape[0]
    heads = lambdas.shape[0]
    fs_rows = key_master.shape[0]
    half = tokens // cores
    rings = rings_from(FIRST_CHIP, chips, cores)
    gather_rings = rings_from(GATHER_CHIP, chips, cores)
    whole = [[rings[c][z] for z in range(chips) for c in core_order(cores)]]
    order = [(FIRST_PLANE + f) % fs_size for f in range(fs_size)]
    planes = [[f * cores + c for f in order for c in core_order(cores)]]
    share = half // chips

    core = lax.axis_index("tp_1")
    came = lax.ppermute(normed, "tp_1", [(0, 1), (1, 0)])
    came = with_layout_constraint(came, Layout(major_to_minor=(0, 1)))
    kept, came = (
        lax.dynamic_slice_in_dim(side, core * half, half, 1, allow_negative_indices=False)
        for side in (normed, came)
    )
    features = jnp.concatenate([kept, came], axis=0)

    by_token = features.T.reshape(chips, share, cores * width)
    by_token, lambdas, first_map, second_map, factor, key_master, value_master = (
        lax.optimization_barrier((
            by_token,
            lambdas,
            first_map,
            second_map,
            factor,
            key_master,
            value_master,
        ))
    )
    by_token = swap(by_token, TP, rings)

    rows_here = lax.axis_index(TP) * width + lax.iota(jnp.int32, width)
    owners = rows_here // VALUE_DIM
    picked = (owners[:, None] == lax.iota(jnp.int32, heads)[None, :]).astype(jnp.float32)
    row_lambda = jnp.sum(picked * lambdas[None, :], axis=1)
    value_cot = (
        first_map.astype(jnp.float32) - row_lambda[:, None] * second_map.astype(jnp.float32)
    ).astype(jnp.bfloat16)
    stacked = jnp.concatenate([key_cot, value_cot], axis=0)
    kept = lax.dynamic_slice_in_dim(stacked, core * half, half, 1)
    sent = lax.dynamic_slice_in_dim(stacked, (1 - core) * half, half, 1)
    masters_here = jnp.concatenate([key_master.T, value_master.T], axis=0)
    masters = jnp.broadcast_to(masters_here[None], (fs_size, *masters_here.shape))
    factor = jnp.roll(factor, -FIRST_PLANE * (rank // fs_size), axis=1)
    gram = lax.dot_general(
        factor, factor, (((0,), (0,)), ((), ())), preferred_element_type=jnp.float32
    )
    blocks = factor.reshape(chips, cores, width, rank)
    own_first = jnp.where(core == 0, blocks, blocks[:, ::-1])
    own_first = jnp.roll(own_first, -FIRST_CHIP, axis=0).reshape(rows, rank)
    fs_at = lax.axis_index(FS) * fs_rows
    masters, gram, own_first, fs_at, sent = lax.optimization_barrier(
        (masters, gram, own_first, fs_at, sent)
    )
    came = lax.ppermute(sent, "tp_1", [(0, 1), (1, 0)])
    is_first = core == FIRST_CORE
    cots = jnp.concatenate([jnp.where(is_first, kept, came), jnp.where(is_first, came, kept)])
    cots = jnp.roll(cots, (FIRST_CHIP - GATHER_CHIP) % chips * share - half, axis=1)
    cots, masters, by_token = lax.optimization_barrier((cots, masters, by_token))
    product = lax.dot_general(
        by_token.transpose(1, 0, 2).reshape(share, rows),
        own_first,
        (((1,), (0,)), ((), ())),
        preferred_element_type=jnp.float32,
    )
    link = (product * LINK_SCALE).astype(jnp.float16)
    masters = swap(masters, FS, [order])
    link = lax.all_gather(link, TP, axis=0, tiled=True, axis_index_groups=gather_rings)

    high, low = in_bf16_parts(link.astype(jnp.float32), 2)
    dims = (((0,), (1,)), ((), ()))
    partial = lax.dot_general(high, cots, dims, preferred_element_type=jnp.float32)
    partial = partial + lax.dot_general(low, cots, dims, preferred_element_type=jnp.float32)
    pieces = partial.reshape(fs_size, rank // fs_size, cores, 2 * width)
    pieces = pieces.transpose(0, 2, 1, 3).reshape(fs_size * cores, rank // fs_size, 2 * width)
    masters, pieces = lax.optimization_barrier((masters, pieces))
    norm_scale = 1.0 / (LINK_SCALE * math.sqrt(tokens * fs_size))
    small = jnp.sum(swap(pieces, FS_CORE, planes), axis=0) * norm_scale

    first = jnp.concatenate([key_first, value_first], axis=1)
    second = jnp.concatenate([key_second, value_second], axis=1)
    first_new = 0.8 * first + 0.2 * small
    second_new = 0.9 * second + 0.1 * small * small
    direction = first_new / (jnp.sqrt(second_new) + 1e-06)
    directions = to_all(direction, FS, [order]).reshape(rank, 2 * width)

    seen = jnp.dot(gram, directions, precision=lax.Precision.HIGHEST)
    squares = jnp.sum(directions * seen, axis=0, keepdims=True)
    squares = jnp.broadcast_to(squares[None], (cores * chips, 1, 2 * width))
    directions, squares, masters, first_new, second_new = lax.optimization_barrier(
        (directions, squares, masters, first_new, second_new)
    )
    squares = swap(squares, TP, whole)
    raw = sum(
        lax.dot_general(part, factor, (((0,), (1,)), ((), ())), preferred_element_type=jnp.float32)
        for part in in_bf16_parts(directions, 3)
    )
    raw_here = lax.dynamic_slice_in_dim(raw, fs_at, fs_rows, 1, allow_negative_indices=False)
    all_masters = jnp.roll(masters, FIRST_PLANE, axis=0).transpose(1, 0, 2).reshape(2 * width, rows)
    squares = jnp.sum(squares.reshape(cores * chips, 2, width), axis=(0, 2))
    cells = rows * width * cores * chips
    scales = 0.02 / jnp.sqrt(squares / cells + 0.01)

    raw, raw_here, all_masters = lax.optimization_barrier((raw, raw_here, all_masters))
    row_scale = lax.optimization_barrier(jnp.repeat(scales, width)[:, None])
    new, copies = [], []
    for at in (0, width):
        span = slice(at, at + width)
        scale = row_scale[span]
        new.append((0.998 * masters_here[span] - scale * raw_here[span]).T)
        copies.append((0.998 * all_masters[span] - scale * raw[span]).astype(jnp.bfloat16).T)
    return (
        *new,
        *copies,
        first_new[:, :width],
        second_new[:, :width],
        first_new[:, width:],
        second_new[:, width:],
    )


def solution(mesh):
    split = Mesh(mesh.devices.reshape(4, 4, 16, 2), ("fs_0", "fs_1", "tp_0", "tp_1"))
    placed = (
        P(TP, FS),
        P(TP, FS),
        P(TP, FS),
        P(TP, FS),
        P(),
        P(),
        P(FS, TP),
        P(FS, TP),
        P(FS, TP),
        P(FS, TP),
        P(FS, TP),
        P(FS, TP),
    )
    return jax.shard_map(
        local,
        mesh=split,
        in_specs=placed,
        out_specs=(
            P(FS, TP),
            P(FS, TP),
            P(None, TP),
            P(None, TP),
            P(FS, TP),
            P(FS, TP),
            P(FS, TP),
            P(FS, TP),
        ),
        check_vma=False,
    )
```

```python
import math

import jax
import jax.numpy as jnp
from jax import lax
from jax.experimental.layout import Layout, with_layout_constraint
from jax.sharding import Mesh
from jax.sharding import PartitionSpec as P

VALUE_DIM = 256
TP = ("tp_0", "tp_1")
FS = ("fs_0", "fs_1")
FS_CORE = ("fs_0", "fs_1", "tp_1")
LINK_SCALE = 32.0
FIRST_CHIP = 9
FIRST_CORE = 1
FIRST_PLANE = 10


def swap(pieces, axes, groups=None):
    return lax.all_to_all(pieces, axes, 0, 0, tiled=True, axis_index_groups=groups)


def to_all(shard, axes, groups):
    size = lax.axis_size(axes)
    return swap(jnp.broadcast_to(shard[None], (size, *shard.shape)), axes, groups)


def core_order(cores):
    return [(FIRST_CORE + c) % cores for c in range(cores)]


def rings_from(first, chips, cores):
    return [[(first + z) % chips * cores + c for z in range(chips)] for c in range(cores)]


def in_bf16_parts(values, count):
    parts = []
    for _ in range(count):
        part = lax.reduce_precision(values, 8, 7)
        parts.append(part.astype(jnp.bfloat16))
        values = values - part
    return parts


def local(
    normed,
    key_cot,
    first_map,
    second_map,
    lambdas,
    factor,
    key_master,
    value_master,
    key_first,
    key_second,
    value_first,
    value_second,
):
    width, tokens = normed.shape
    cores = lax.axis_size("tp_1")
    chips = lax.axis_size("tp_0")
    fs_size = lax.axis_size(FS)
    rank = factor.shape[1]
    rows = factor.shape[0]
    heads = lambdas.shape[0]
    fs_rows = key_master.shape[0]
    half = tokens // cores
    rings = rings_from(FIRST_CHIP, chips, cores)
    whole = [[rings[c][z] for z in range(chips) for c in core_order(cores)]]
    order = [(FIRST_PLANE + f) % fs_size for f in range(fs_size)]
    planes = [[f * cores + c for f in order for c in core_order(cores)]]
    share = half // chips

    core = lax.axis_index("tp_1")
    came = lax.ppermute(normed, "tp_1", [(0, 1), (1, 0)])
    came = with_layout_constraint(came, Layout(major_to_minor=(0, 1)))
    kept, came = (
        lax.dynamic_slice_in_dim(side, core * half, half, 1, allow_negative_indices=False)
        for side in (normed, came)
    )
    features = jnp.concatenate([kept, came], axis=0)

    by_token = features.T.reshape(chips, share, cores * width)
    by_token, lambdas, first_map, second_map, factor, key_master, value_master = (
        lax.optimization_barrier((
            by_token,
            lambdas,
            first_map,
            second_map,
            factor,
            key_master,
            value_master,
        ))
    )
    by_token = swap(by_token, TP, rings)

    rows_here = lax.axis_index(TP) * width + lax.iota(jnp.int32, width)
    owners = rows_here // VALUE_DIM
    picked = (owners[:, None] == lax.iota(jnp.int32, heads)[None, :]).astype(jnp.float32)
    row_lambda = jnp.sum(picked * lambdas[None, :], axis=1)
    value_cot = (
        first_map.astype(jnp.float32) - row_lambda[:, None] * second_map.astype(jnp.float32)
    ).astype(jnp.bfloat16)
    stacked = jnp.concatenate([key_cot, value_cot], axis=0)
    kept = lax.dynamic_slice_in_dim(stacked, core * half, half, 1)
    sent = lax.dynamic_slice_in_dim(stacked, (1 - core) * half, half, 1)
    masters_here = jnp.concatenate([key_master.T, value_master.T], axis=0)
    masters = jnp.broadcast_to(masters_here[None], (fs_size, *masters_here.shape))
    factor = jnp.roll(factor, -FIRST_PLANE * (rank // fs_size), axis=1)
    gram = lax.dot_general(
        factor, factor, (((0,), (0,)), ((), ())), preferred_element_type=jnp.float32
    )
    blocks = factor.reshape(chips, cores, width, rank)
    own_first = jnp.where(core == 0, blocks, blocks[:, ::-1])
    own_first = jnp.roll(own_first, -FIRST_CHIP, axis=0).reshape(rows, rank)
    fs_at = lax.axis_index(FS) * fs_rows
    masters, gram, own_first, fs_at, sent = lax.optimization_barrier(
        (masters, gram, own_first, fs_at, sent)
    )
    came = lax.ppermute(sent, "tp_1", [(0, 1), (1, 0)])
    is_first = core == FIRST_CORE
    cots = jnp.concatenate([jnp.where(is_first, kept, came), jnp.where(is_first, came, kept)])
    cots, masters, by_token = lax.optimization_barrier((cots, masters, by_token))
    product = lax.dot_general(
        by_token.transpose(1, 0, 2).reshape(share, rows),
        own_first,
        (((1,), (0,)), ((), ())),
        preferred_element_type=jnp.float32,
    )
    link = (product * LINK_SCALE).astype(jnp.float16)
    masters = swap(masters, FS, [order])
    link = lax.all_gather(link, TP, axis=0, tiled=True, axis_index_groups=rings)

    high, low = in_bf16_parts(link.astype(jnp.float32), 2)
    dims = (((0,), (1,)), ((), ()))
    partial = lax.dot_general(high, cots, dims, preferred_element_type=jnp.float32)
    partial = partial + lax.dot_general(low, cots, dims, preferred_element_type=jnp.float32)
    pieces = partial.reshape(fs_size, rank // fs_size, cores, 2 * width)
    pieces = pieces.transpose(0, 2, 1, 3).reshape(fs_size * cores, rank // fs_size, 2 * width)
    masters, pieces = lax.optimization_barrier((masters, pieces))
    norm_scale = 1.0 / (LINK_SCALE * math.sqrt(tokens * fs_size))
    small = jnp.sum(swap(pieces, FS_CORE, planes), axis=0) * norm_scale

    first = jnp.concatenate([key_first, value_first], axis=1)
    second = jnp.concatenate([key_second, value_second], axis=1)
    first_new = 0.8 * first + 0.2 * small
    second_new = 0.9 * second + 0.1 * small * small
    direction = first_new / (jnp.sqrt(second_new) + 1e-06)
    directions = to_all(direction, FS, [order]).reshape(rank, 2 * width)

    seen = jnp.dot(gram, directions, precision=lax.Precision.HIGHEST)
    squares = jnp.sum(directions * seen, axis=0, keepdims=True)
    squares = jnp.broadcast_to(squares[None], (cores * chips, 1, 2 * width))
    directions, squares, masters, first_new, second_new = lax.optimization_barrier(
        (directions, squares, masters, first_new, second_new)
    )
    squares = swap(squares, TP, whole)
    raw = sum(
        lax.dot_general(part, factor, (((0,), (1,)), ((), ())), preferred_element_type=jnp.float32)
        for part in in_bf16_parts(directions, 3)
    )
    raw_here = lax.dynamic_slice_in_dim(raw, fs_at, fs_rows, 1, allow_negative_indices=False)
    all_masters = jnp.roll(masters, FIRST_PLANE, axis=0).transpose(1, 0, 2).reshape(2 * width, rows)
    squares = jnp.sum(squares.reshape(cores * chips, 2, width), axis=(0, 2))
    cells = rows * width * cores * chips
    scales = 0.02 / jnp.sqrt(squares / cells + 0.01)

    raw, raw_here, all_masters = lax.optimization_barrier((raw, raw_here, all_masters))
    row_scale = lax.optimization_barrier(jnp.repeat(scales, width)[:, None])
    new, copies = [], []
    for at in (0, width):
        span = slice(at, at + width)
        scale = row_scale[span]
        new.append((0.998 * masters_here[span] - scale * raw_here[span]).T)
        copies.append((0.998 * all_masters[span] - scale * raw[span]).astype(jnp.bfloat16).T)
    return (
        *new,
        *copies,
        first_new[:, :width],
        second_new[:, :width],
        first_new[:, width:],
        second_new[:, width:],
    )


def solution(mesh):
    split = Mesh(mesh.devices.reshape(4, 4, 16, 2), ("fs_0", "fs_1", "tp_0", "tp_1"))
    placed = (
        P(TP, FS),
        P(TP, FS),
        P(TP, FS),
        P(TP, FS),
        P(),
        P(),
        P(FS, TP),
        P(FS, TP),
        P(FS, TP),
        P(FS, TP),
        P(FS, TP),
        P(FS, TP),
    )
    return jax.shard_map(
        local,
        mesh=split,
        in_specs=placed,
        out_specs=(
            P(FS, TP),
            P(FS, TP),
            P(None, TP),
            P(None, TP),
            P(FS, TP),
            P(FS, TP),
            P(FS, TP),
            P(FS, TP),
        ),
        check_vma=False,
    )
```
